32 devices in a mesh: sp: 4 (over z), dp: 8 (over y, x, core).
Axes of the slice: x: 2, y: 2, z: 4, core: 2. Of those that a mesh axis runs over, the one named last changes fastest.
Arguments:
- mixing_input: bfloat16 [8, 512, 2048], P('dp', 'sp'), may hold values from -6 to 6
- cotangent: bfloat16 [8, 512, 2048], P('dp', 'sp'), may hold values from -6 to 6
- filter_taps: bfloat16 [4, 2048], P(None, 'sp'), may hold values from -3 to 3
- recurrence_gate_map: bfloat16 [2, 16, 128, 128], P(None, 'sp'), may hold values from -0.5 to 0.5
- input_gate_map: bfloat16 [2, 16, 128, 128], P(None, 'sp'), may hold values from -0.5 to 0.5
- decay_logit_param: float32 [2, 2048], P(None, 'sp')
- spike_decay: float32 [8, 16, 512], P('dp', 'sp'), may hold values from -2 to -0.0001953125
Outputs:
- grad_input: bfloat16 [8, 512, 2048], P('dp', 'sp')
- grad_rate_map: float32 [2, 16, 128, 128], P(None, 'sp')
- grad_input_map: float32 [2, 16, 128, 128], P(None, 'sp')
- grad_conv_taps: float32 [4, 2048], P(None, 'sp')
The draws below stay inside these ranges and needn't reach their ends.
All inputs are finite; a program needn't handle non-finite values.
Results may differ from the reference program's by a relative error of at most 0.0075.
Values may be sent and summed in bfloat16 or wider, within the bound.
A program may use at most 64 MiB of HBM per device.

```python
import math
import jax
import jax.numpy as jnp
from jax import lax

HEAD = 128
HEAD_COUNT = 16
CONV = 4
TOK_DEV = 128
WIDTH = 2048
SEQUENCE_LENGTH = 512
BATCH_COUNT = 8


def draw_decay_logit_param(key, part):
    pick_key = jax.random.fold_in(key, 11)
    fast_key = jax.random.fold_in(key, 12)
    slow_key = jax.random.fold_in(key, 13)
    picked = jax.random.uniform(pick_key, (2, HEAD_COUNT, 1), jnp.float32)
    fast_heads = picked < 0.5
    fast_keep = jax.random.uniform(fast_key, (2, HEAD_COUNT, HEAD), jnp.float32, 0.004, 0.008)
    slow_keep = jax.random.uniform(slow_key, (2, HEAD_COUNT, HEAD), jnp.float32, 0.1, 0.4) / (4.0 * SEQUENCE_LENGTH)
    retain = jnp.where(fast_heads, fast_keep, slow_keep)
    return (-jnp.log(jnp.expm1(retain))).reshape(2, HEAD_COUNT * HEAD)


def draw_spike_decay(key, part):
    base_key = jax.random.fold_in(key, 21)
    position_key = jax.random.fold_in(key, 22)
    loss_key = jax.random.fold_in(key, 23)
    low_end = 0.25
    high_end = 1.0
    blocks = SEQUENCE_LENGTH // TOK_DEV
    baseline_rate = jnp.exp(jax.random.uniform(base_key, (BATCH_COUNT, HEAD_COUNT, blocks), jnp.float32, math.log(low_end), math.log(high_end))) / SEQUENCE_LENGTH
    baseline_rate = jnp.repeat(baseline_rate, TOK_DEV, axis=2)
    spike_positions = jax.random.randint(position_key, (BATCH_COUNT, HEAD_COUNT, 2), 0, SEQUENCE_LENGTH)
    loss_values = jax.random.uniform(loss_key, (BATCH_COUNT, HEAD_COUNT, 2), jnp.float32, 0.2, 0.5)
    position_index = jnp.arange(SEQUENCE_LENGTH)
    spike_events = spike_positions[:, :, :, None] == position_index[None, None, None, :]
    spike_total = jnp.sum(jnp.where(spike_events, jnp.log1p(-loss_values)[:, :, :, None], 0.0), axis=2)
    return spike_total - baseline_rate


def steps_of(stream_key, dims, split, least, high):
    def one(position, blocks):
        draws = jax.random.uniform(jax.random.fold_in(jax.random.fold_in(stream_key, 6), position), (blocks,), jnp.float32, least / len(split), high / len(split))
        return jnp.repeat(jnp.exp(draws), dims[position] // blocks).reshape((-1,) + (1,) * (len(dims) - position - 1))

    factor_of = one(*split[0])
    for cut in split[1:]:
        factor_of = factor_of * one(*cut)
    return factor_of


def gaussian(rng, dims, deviation, reach, split=(), kind=jnp.bfloat16):
    values = jax.random.normal(rng, dims, jnp.float32) * deviation
    if len(split) > 0:
        values = steps_of(rng, dims, split, -0.22, 0.18) * values
    return jnp.clip(values, min=-reach, max=reach).astype(kind)


def setup_inputs(seed: int = 0) -> dict:
    arg_keys = jax.random.split(jax.random.key(seed), 8)
    return {
        "mixing_input": gaussian(arg_keys[0], (BATCH_COUNT, SEQUENCE_LENGTH, WIDTH), 1.0, 6.0, ((0, 8), (1, 4))),
        "cotangent": gaussian(arg_keys[1], (BATCH_COUNT, SEQUENCE_LENGTH, WIDTH), 1.0, 6.0, ((0, 8), (1, 4))),
        "filter_taps": gaussian(arg_keys[2], (CONV, WIDTH), CONV ** -0.5, 3.0, ((1, 4),)),
        "recurrence_gate_map": gaussian(arg_keys[3], (2, HEAD_COUNT, HEAD, HEAD), HEAD ** -0.5, 0.5, ((1, 4),)),
        "input_gate_map": gaussian(arg_keys[4], (2, HEAD_COUNT, HEAD, HEAD), HEAD ** -0.5, 0.5, ((1, 4),)),
        "decay_logit_param": draw_decay_logit_param(jax.random.fold_in(arg_keys[7], 71), 0),
        "spike_decay": draw_spike_decay(jax.random.fold_in(arg_keys[7], 71), 0),
    }


decay_multiplier_value = 8.0

def forward_scan(coefficient, source):

    def combine(earlier, second):
        return (earlier[0] * second[0], second[0] * earlier[1] + second[1])
    return lax.associative_scan(combine, (coefficient, source), axis=0)[1]

def reverse_scan(coefficient, source):

    def combine(earlier, second):
        return (earlier[0] * second[0], second[0] * earlier[1] + second[1])
    return lax.associative_scan(combine, (coefficient, source), axis=0, reverse=True)[1]

def shift_down(signal):
    return jnp.concatenate([jnp.zeros_like(signal[:1]), signal[:-1]], axis=0)

def shift_up(signal):
    return jnp.concatenate([signal[1:], jnp.zeros_like(signal[:1])], axis=0)

def convolve(signal, kernel_taps):
    length = signal.shape[0]
    padded = jnp.pad(signal, ((2, 1), (0, 0), (0, 0)))
    running = padded[0:length] * kernel_taps[0]
    for offset in range(1, 4):
        running = running + padded[offset:offset + length] * kernel_taps[offset]
    return running

def convolve_back(signal, kernel_taps):
    length = signal.shape[0]
    padded = jnp.pad(signal, ((1, 2), (0, 0), (0, 0)))
    running = padded[3:3 + length] * kernel_taps[0]
    for offset in range(1, 4):
        running = running + padded[3 - offset:3 - offset + length] * kernel_taps[offset]
    return running

def tap_gradients(signal, value_grad):
    length = signal.shape[0]
    padded = jnp.pad(signal, ((2, 1), (0, 0), (0, 0)))
    return jnp.stack([lax.optimization_barrier(jnp.sum(padded[offset:offset + length] * value_grad, axis=0)) for offset in range(4)])

def directional_terms(lower_values, upstream_field, recurrence_weight, input_gate_weight, decay_logit_rows, spike_rows, backward_step):
    conv_values = lower_values.astype(jnp.float32)
    rate_wide = recurrence_weight.astype(jnp.float32)
    input_wide = input_gate_weight.astype(jnp.float32)
    recurrence_gate = jax.nn.sigmoid(jnp.einsum('thi,hij->thj', conv_values, rate_wide))
    input_gate = jax.nn.sigmoid(jnp.einsum('thi,hij->thj', conv_values, input_wide))
    logarithm_keep = jax.nn.log_sigmoid(decay_logit_rows)
    logarithm_decay = decay_multiplier_value * recurrence_gate * logarithm_keep + spike_rows[:, :, None]
    decay_factor = jnp.exp(logarithm_decay)
    multiplier = jnp.sqrt(-jnp.expm1(2.0 * logarithm_decay))
    source = multiplier * input_gate * conv_values
    if backward_step:
        hidden_state = reverse_scan(decay_factor, source)
        adjoint = forward_scan(shift_down(decay_factor), upstream_field)
        before = shift_up(hidden_state)
    else:
        hidden_state = forward_scan(decay_factor, source)
        adjoint = reverse_scan(shift_up(decay_factor), upstream_field)
        before = shift_down(hidden_state)
    log_grad = adjoint * before * decay_factor - adjoint * input_gate * conv_values * decay_factor * decay_factor / multiplier
    rate_back = lax.optimization_barrier((log_grad * decay_multiplier_value * logarithm_keep * recurrence_gate * (1.0 - recurrence_gate)).astype(jnp.bfloat16))
    gate_back = lax.optimization_barrier((adjoint * multiplier * conv_values * input_gate * (1.0 - input_gate)).astype(jnp.bfloat16))
    rate_back_wide = rate_back.astype(jnp.float32)
    gate_back_wide = gate_back.astype(jnp.float32)
    value_grad = adjoint * multiplier * input_gate
    value_grad = value_grad + jnp.einsum('thj,hij->thi', rate_back_wide, rate_wide)
    value_grad = value_grad + jnp.einsum('thj,hij->thi', gate_back_wide, input_wide)
    rate_gradient = jnp.einsum('thi,thj->hij', conv_values, rate_back_wide)
    gate_gradient = jnp.einsum('thi,thj->hij', conv_values, gate_back_wide)
    return (value_grad, rate_gradient, gate_gradient)

def reference(mixing_input, cotangent, filter_taps, recurrence_gate_map, input_gate_map, decay_logit_param, spike_decay):
    kernel_taps = filter_taps.astype(jnp.float32).reshape(CONV, HEAD_COUNT, HEAD)
    decay_logit_rows = decay_logit_param.reshape(2, HEAD_COUNT, HEAD)
    norm_factor = (BATCH_COUNT * SEQUENCE_LENGTH) ** (-0.5)

    def single_sequence(total_sums, sequence_items):
        input_rows, output_gradients, spike_values = sequence_items
        signal = input_rows.astype(jnp.float32).reshape(SEQUENCE_LENGTH, HEAD_COUNT, HEAD)
        lower_values = lax.optimization_barrier(convolve(signal, kernel_taps).astype(jnp.bfloat16))
        upstream_field = output_gradients.astype(jnp.float32).reshape(SEQUENCE_LENGTH, HEAD_COUNT, HEAD)
        spike_rows = jnp.transpose(spike_values)
        value_grad = jnp.zeros((SEQUENCE_LENGTH, HEAD_COUNT, HEAD), jnp.float32)
        rate_parts = []
        gate_parts = []
        for scan_direction in range(2):
            value_portion, rate_gradient, gate_gradient = directional_terms(lower_values, upstream_field, recurrence_gate_map[scan_direction], input_gate_map[scan_direction], decay_logit_rows[scan_direction], spike_rows, scan_direction == 1)
            value_grad = value_grad + value_portion
            rate_parts.append(rate_gradient)
            gate_parts.append(gate_gradient)
        input_grad = convolve_back(value_grad, kernel_taps).astype(jnp.bfloat16).reshape(SEQUENCE_LENGTH, HEAD_COUNT * HEAD)
        tap_part = tap_gradients(signal, value_grad)
        total_sums = (total_sums[0] + jnp.stack(rate_parts), total_sums[1] + jnp.stack(gate_parts), total_sums[2] + tap_part)
        return (total_sums, input_grad)
    starting_state = (jnp.zeros((2, HEAD_COUNT, HEAD, HEAD), jnp.float32), jnp.zeros((2, HEAD_COUNT, HEAD, HEAD), jnp.float32), jnp.zeros((CONV, HEAD_COUNT, HEAD), jnp.float32))
    total_sums, input_gradients = lax.scan(single_sequence, starting_state, (mixing_input, cotangent, spike_decay))
    return (input_gradients, total_sums[0] * norm_factor, total_sums[1] * norm_factor, (total_sums[2] * norm_factor).reshape(CONV, HEAD_COUNT * HEAD))
```

```python
import functools
import math

import jax
import jax.numpy as jnp
from jax import lax
from jax.experimental import pallas as pl
from jax.experimental.pallas import tpu as pltpu
from jax.sharding import PartitionSpec as P

SEG = 8
LANES = 128
UNROLL = 4


def shift_segments(rows, down):
    index = lax.broadcasted_iota(jnp.int32, rows.shape, 0)
    if down:
        return jnp.where(index == 0, 0.0, pltpu.roll(rows, 1, 0))
    return jnp.where(index == SEG - 1, 0.0, pltpu.roll(rows, SEG - 1, 0))


def carry_in(product, total, down):
    p = shift_segments(product, down)
    q = shift_segments(total, down)
    for step in (1, 2, 4):
        amount = step if down else SEG - step
        q = q + p * pltpu.roll(q, amount, 0)
        p = p * pltpu.roll(p, amount, 0)
    return q


def load_head(x_ref, c_ref, s, rows):
    pitch = rows + SEG
    for seg in range(SEG):
        s["xs"][pl.ds(seg * pitch, rows), :] = x_ref[pl.ds(seg * rows, rows), :].astype(jnp.float32)
        s["cs"][pl.ds(seg * pitch, rows), :] = c_ref[pl.ds(seg * rows, rows), :].astype(jnp.float32)


def head_compute(s, rows, spike_ref, taps, keep, weights, out_gi):
    f32, bf16 = jnp.float32, jnp.bfloat16
    pitch = rows + SEG
    length = rows * SEG
    tile = (SEG, LANES)
    tap = [jnp.broadcast_to(taps[k : k + 1, :], tile) for k in range(4)]
    logit = keep
    log_keep = jnp.minimum(logit, 0.0) - jnp.log1p(jnp.exp(-jnp.abs(logit)))
    k4 = [jnp.broadcast_to(4.0 * log_keep[d : d + 1, :], tile) for d in range(2)]
    k2 = [jnp.broadcast_to(2.0 * log_keep[d : d + 1, :], tile) for d in range(2)]

    for j in range(4):
        s["wc"][:, j * LANES : (j + 1) * LANES] = weights[j]()
    for b in range(length // LANES):
        s["spk"][pl.ds(b * (LANES // SEG), LANES // SEG)] = jnp.transpose(
            jnp.broadcast_to(spike_ref[b : b + 1, :], (LANES, LANES))
        ).reshape(LANES // SEG, SEG, LANES)

    def permute(i, _):
        for u in range(UNROLL):
            r = i * UNROLL + u
            s["xp"][r + 2] = s["xs"][pl.ds(r, SEG, stride=pitch), :]
            s["cp"][r] = s["cs"][pl.ds(r, SEG, stride=pitch), :]
        return 0

    lax.fori_loop(0, rows // UNROLL, permute, 0)
    xp = s["xp"]
    xp[0] = shift_segments(xp[rows], True)
    xp[1] = shift_segments(xp[rows + 1], True)
    xp[rows + 2] = shift_segments(xp[2], False)

    def conv(i, _):
        for u in range(0, UNROLL, 2):
            r = i * UNROLL + u
            pair = []
            for w in range(2):
                acc = xp[r + w] * tap[0]
                for k in range(1, 4):
                    acc = acc + xp[r + w + k] * tap[k]
                pair.append(acc)
            start = pl.multiple_of(r * SEG, 2 * SEG)
            s["vb"][pl.ds(start, 2 * SEG), :] = jnp.concatenate(pair, axis=0).astype(bf16)
        return 0

    lax.fori_loop(0, rows // UNROLL, conv, 0)

    chunk = 256

    def gates(i, _):
        start = pl.multiple_of(i * chunk, chunk)
        s["pre"][pl.ds(start, chunk), :] = jnp.dot(
            s["vb"][pl.ds(start, chunk), :], s["wc"][...], preferred_element_type=f32
        )
        return 0

    lax.fori_loop(0, length // chunk, gates, 0)

    def first(i, carry):
        p0, s0, w0, p1, s1, w1 = carry
        for u in range(0, UNROLL, 2):
            base = i * UNROLL + u
            start = pl.multiple_of(base * SEG, 2 * SEG)
            v_pair = s["vb"][pl.ds(start, 2 * SEG), :].astype(f32)
            for w in range(2):
                r = base + w
                row = pl.multiple_of(r * SEG, SEG)
                v = v_pair[w * SEG : (w + 1) * SEG]
                c = s["cp"][r]
                spike = s["spk"][r]
                found = []
                for d in range(2):
                    th = jnp.tanh(0.5 * s["pre"][pl.ds(row, SEG), 2 * d * LANES : (2 * d + 1) * LANES])
                    tg = jnp.tanh(0.5 * s["pre"][pl.ds(row, SEG), (2 * d + 1) * LANES : (2 * d + 2) * LANES])
                    log_decay = k4[d] * th + (k4[d] + spike)
                    decay = jnp.exp(log_decay)
                    decay2 = decay * decay
                    m2 = -jnp.tanh(log_decay) * (1.0 + decay2)
                    inverse = lax.rsqrt(m2)
                    half = 0.5 * tg
                    gate = 0.5 + half
                    slope = (m2 * inverse) * gate
                    source = slope * v
                    s["dec"][d, r] = decay
                    s["src"][d, r] = source
                    s["slope"][d, r] = slope
                    s["second"][d, r] = gate * v * decay2 * inverse
                    s["rate"][d, r] = k2[d] * (1.0 - th * th)
                    s["gate"][d, r] = source * (0.5 - half)
                    found.append((decay, source))
                (d0, g0), (d1, g1) = found
                s0 = d0 * s0 + g0
                p0 = p0 * d0
                w0 = w0 + p0 * c
                w1 = d1 * (c + w1)
                s1 = s1 + p1 * g1
                p1 = p1 * d1
        return p0, s0, w0, p1, s1, w1

    zero = jnp.zeros(tile, f32)
    one = jnp.ones(tile, f32)
    p0, s0, w0, p1, s1, w1 = lax.fori_loop(0, rows // UNROLL, first, (one, zero, zero, one, zero, zero))
    s0 = carry_in(p0, s0, True)
    w0 = carry_in(p0, w0, False)
    w1 = carry_in(p1, w1, True)
    s1 = carry_in(p1, s1, False)

    def forward(i, carry):
        state, back = carry
        for u in range(UNROLL):
            r = i * UNROLL + u
            moved = s["dec"][0, r] * state
            state = moved + s["src"][0, r]
            s["rate"][0, r] = (moved - s["second"][0, r]) * s["rate"][0, r]
            adjoint = s["cp"][r] + back
            back = s["dec"][1, r] * adjoint
            s["adj"][r] = adjoint
        return state, back

    lax.fori_loop(0, rows // UNROLL, forward, (s0, w1))

    def reverse(i, carry):
        state, back = carry
        for u in range(UNROLL - 2, -2, -2):
            base = rows - (i + 1) * UNROLL + u
            parts = [None, None]
            for w in (1, 0):
                r = base + w
                adjoint = s["cp"][r] + back
                back = s["dec"][0, r] * adjoint
                moved = s["dec"][1, r] * state
                state = moved + s["src"][1, r]
                other = s["adj"][r]
                s["vg"][r + 1] = adjoint * s["slope"][0, r] + other * s["slope"][1, r]
                parts[w] = (
                    adjoint * s["rate"][0, r],
                    adjoint * s["gate"][0, r],
                    other * ((moved - s["second"][1, r]) * s["rate"][1, r]),
                    other * s["gate"][1, r],
                )
            start = pl.multiple_of(base * SEG, 2 * SEG)
            for j in range(4):
                s["back"][pl.ds(start, 2 * SEG), j * LANES : (j + 1) * LANES] = jnp.concatenate(
                    [parts[0][j], parts[1][j]], axis=0
                ).astype(bf16)
        return state, back

    lax.fori_loop(0, rows // UNROLL, reverse, (s1, w0))

    vg = s["vg"]

    def through(i, _):
        start = pl.multiple_of(i * chunk, chunk)
        part = lax.dot_general(
            s["back"][pl.ds(start, chunk), :],
            s["wc"][...],
            (((1,), (1,)), ((), ())),
            preferred_element_type=f32,
        )
        where = pl.ds(i * (chunk // SEG) + 1, chunk // SEG)
        vg[where] = vg[where] + part.reshape(chunk // SEG, SEG, LANES)
        return 0

    lax.fori_loop(0, length // chunk, through, 0)
    vg[0] = shift_segments(vg[rows], True)
    vg[rows + 1] = shift_segments(vg[1], False)
    vg[rows + 2] = shift_segments(vg[2], False)

    maps = lax.dot_general(
        s["vb"][...], s["back"][...], (((0,), (0,)), ((), ())), preferred_element_type=f32
    )

    def last(i, sums):
        sums = list(sums)
        for u in range(UNROLL):
            r = i * UNROLL + u
            here = vg[r + 1]
            acc = vg[r + 3] * tap[0] + vg[r + 2] * tap[1] + here * tap[2] + vg[r] * tap[3]
            s["xs"][pl.ds(r, SEG, stride=pitch), :] = acc
            for k in range(4):
                sums[k] = sums[k] + xp[r + k] * here
        return tuple(sums)

    sums = lax.fori_loop(0, rows // UNROLL, last, (zero,) * 4)
    for seg in range(SEG):
        out_gi(seg, s["xs"][pl.ds(seg * pitch, rows), :].astype(bf16))
    tap_rows = jnp.concatenate([jnp.sum(a, axis=0, keepdims=True) for a in sums], axis=0)
    return maps, tap_rows


def head_scratch(rows):
    f32, bf16 = jnp.float32, jnp.bfloat16
    length = rows * SEG
    pitch = rows + SEG
    per = lambda n: pltpu.VMEM((n, SEG, LANES), f32)
    both = lambda: pltpu.VMEM((2, rows, SEG, LANES), f32)
    return dict(
        xs=pltpu.VMEM((SEG * pitch, LANES), f32),
        cs=pltpu.VMEM((SEG * pitch, LANES), f32),
        xp=per(rows + 3),
        cp=per(rows),
        spk=per(rows),
        vb=pltpu.VMEM((length, LANES), bf16),
        wc=pltpu.VMEM((LANES, 4 * LANES), bf16),
        pre=pltpu.VMEM((length, 4 * LANES), f32),
        dec=both(),
        src=both(),
        slope=both(),
        second=both(),
        rate=both(),
        gate=both(),
        adj=per(rows),
        vg=per(rows + 3),
        back=pltpu.VMEM((length, 4 * LANES), bf16),
    )


def head_kernel(rows, norm, x_ref, c_ref, taps_ref, rmap_ref, imap_ref, keep_ref, spike_ref,
                gi_ref, grate_ref, ginput_ref, gtaps_ref, s):
    load_head(x_ref, c_ref, s, rows)

    def out_gi(seg, value):
        gi_ref[pl.ds(seg * rows, rows), :] = value

    weights = [
        lambda: rmap_ref[0, 0], lambda: imap_ref[0, 0],
        lambda: rmap_ref[1, 0], lambda: imap_ref[1, 0],
    ]
    maps, tap_rows = head_compute(
        s, rows, spike_ref.at[0], taps_ref[...], keep_ref[...], weights, out_gi
    )
    maps = maps * norm
    for d in range(2):
        grate_ref[d, 0] = maps[:, 2 * d * LANES : (2 * d + 1) * LANES]
        ginput_ref[d, 0] = maps[:, (2 * d + 1) * LANES : (2 * d + 2) * LANES]
    gtaps_ref[...] = tap_rows * norm


def body(mixing_input, cotangent, filter_taps, recurrence_gate_map, input_gate_map,
         decay_logit_param, spike_decay):
    heads = recurrence_gate_map.shape[1]
    seq_x = lax.all_to_all(mixing_input, "sp", split_axis=2, concat_axis=1, tiled=True)[0]
    seq_c = lax.all_to_all(cotangent, "sp", split_axis=2, concat_axis=1, tiled=True)[0]
    length, width = seq_x.shape
    rows = length // SEG
    norm = 1.0 / math.sqrt(lax.axis_size("dp") * length)
    taps = filter_taps.astype(jnp.float32)
    spike = jnp.swapaxes(spike_decay[0].reshape(heads, SEG, rows), 1, 2)
    spike = spike.reshape(heads, length // LANES, LANES)
    f32 = jnp.float32
    gi, grate, ginput, gtaps = pl.pallas_call(
        functools.partial(head_kernel, rows, norm),
        grid=(heads,),
        in_specs=[
            pl.BlockSpec((length, LANES), lambda h: (0, h)),
            pl.BlockSpec((length, LANES), lambda h: (0, h)),
            pl.BlockSpec((4, LANES), lambda h: (0, h)),
            pl.BlockSpec((2, 1, LANES, LANES), lambda h: (0, h, 0, 0)),
            pl.BlockSpec((2, 1, LANES, LANES), lambda h: (0, h, 0, 0)),
            pl.BlockSpec((2, LANES), lambda h: (0, h)),
            pl.BlockSpec((1, length // LANES, LANES), lambda h: (h, 0, 0)),
        ],
        out_specs=[
            pl.BlockSpec((length, LANES), lambda h: (0, h)),
            pl.BlockSpec((2, 1, LANES, LANES), lambda h: (0, h, 0, 0)),
            pl.BlockSpec((2, 1, LANES, LANES), lambda h: (0, h, 0, 0)),
            pl.BlockSpec((4, LANES), lambda h: (0, h)),
        ],
        out_shape=[
            jax.ShapeDtypeStruct((length, width), jnp.bfloat16),
            jax.ShapeDtypeStruct((2, heads, LANES, LANES), f32),
            jax.ShapeDtypeStruct((2, heads, LANES, LANES), f32),
            jax.ShapeDtypeStruct((4, width), f32),
        ],
        scratch_shapes=[head_scratch(rows)],
        compiler_params=pltpu.CompilerParams(
            dimension_semantics=("arbitrary",), vmem_limit_bytes=50 * 1024 * 1024
        ),
        name="heads",
    )(seq_x, seq_c, taps, recurrence_gate_map, input_gate_map, decay_logit_param, spike)
    grate, ginput, gtaps = lax.psum((grate, ginput, gtaps), "dp")
    grad_input = lax.all_to_all(gi[None], "sp", split_axis=1, concat_axis=2, tiled=True)
    return grad_input, grate, ginput, gtaps


def solution(mesh):
    return jax.shard_map(
        body,
        mesh=mesh,
        in_specs=(
            P("dp", "sp", None),
            P("dp", "sp", None),
            P(None, "sp"),
            P(None, "sp", None, None),
            P(None, "sp", None, None),
            P(None, "sp"),
            P("dp", "sp", None),
        ),
        out_specs=(
            P("dp", "sp", None),
            P(None, "sp", None, None),
            P(None, "sp", None, None),
            P(None, "sp"),
        ),
        check_vma=False,
    )
```

```python
import functools
import math

import jax
import jax.numpy as jnp
from jax import lax
from jax.experimental import pallas as pl
from jax.experimental.pallas import tpu as pltpu
from jax.sharding import PartitionSpec as P

SEG = 8
LANES = 128
UNROLL = 4


def shift_segments(rows, down):
    index = lax.broadcasted_iota(jnp.int32, rows.shape, 0)
    if down:
        return jnp.where(index == 0, 0.0, pltpu.roll(rows, 1, 0))
    return jnp.where(index == SEG - 1, 0.0, pltpu.roll(rows, SEG - 1, 0))


def carry_in(product, total, down):
    p = shift_segments(product, down)
    q = shift_segments(total, down)
    for step in (1, 2, 4):
        amount = step if down else SEG - step
        q = q + p * pltpu.roll(q, amount, 0)
        p = p * pltpu.roll(p, amount, 0)
    return q


def load_head(x_ref, c_ref, s, rows):
    pitch = rows + SEG
    for seg in range(SEG):
        s["xs"][pl.ds(seg * pitch, rows), :] = x_ref[pl.ds(seg * rows, rows), :].astype(jnp.float32)
        s["cs"][pl.ds(seg * pitch, rows), :] = c_ref[pl.ds(seg * rows, rows), :].astype(jnp.float32)


def head_compute(s, rows, spike_row, taps, keep, weights, out_gi):
    f32, bf16 = jnp.float32, jnp.bfloat16
    pitch = rows + SEG
    length = rows * SEG
    tile = (SEG, LANES)
    tap = [jnp.broadcast_to(taps[k : k + 1, :], tile) for k in range(4)]
    logit = keep
    log_keep = jnp.minimum(logit, 0.0) - jnp.log1p(jnp.exp(-jnp.abs(logit)))
    k4 = [jnp.broadcast_to(4.0 * log_keep[d : d + 1, :], tile) for d in range(2)]
    k2 = [jnp.broadcast_to(2.0 * log_keep[d : d + 1, :], tile) for d in range(2)]

    for j in range(4):
        s["wc"][:, j * LANES : (j + 1) * LANES] = weights[j]()
    piece = min(rows, LANES)
    for b in range(length // LANES):
        block = jnp.transpose(
            jnp.broadcast_to(spike_row(b), (LANES, LANES))
        )
        for e in range(LANES // piece):
            at = b * LANES + e * piece
            where = at // rows * pitch + at % rows
            s["ss"][pl.ds(where, piece), :] = block[e * piece : (e + 1) * piece]

    def permute(i, _):
        for u in range(UNROLL):
            r = i * UNROLL + u
            s["xp"][r + 2] = s["xs"][pl.ds(r, SEG, stride=pitch), :]
            s["cp"][r] = s["cs"][pl.ds(r, SEG, stride=pitch), :]
            s["spk"][r] = s["ss"][pl.ds(r, SEG, stride=pitch), :]
        return 0

    lax.fori_loop(0, rows // UNROLL, permute, 0)
    xp = s["xp"]
    xp[0] = shift_segments(xp[rows], True)
    xp[1] = shift_segments(xp[rows + 1], True)
    xp[rows + 2] = shift_segments(xp[2], False)

    def conv(i, _):
        for u in range(0, UNROLL, 2):
            r = i * UNROLL + u
            pair = []
            for w in range(2):
                acc = xp[r + w] * tap[0]
                for k in range(1, 4):
                    acc = acc + xp[r + w + k] * tap[k]
                pair.append(acc)
            start = pl.multiple_of(r * SEG, 2 * SEG)
            s["vb"][pl.ds(start, 2 * SEG), :] = jnp.concatenate(pair, axis=0).astype(bf16)
        return 0

    lax.fori_loop(0, rows // UNROLL, conv, 0)

    chunk = 256

    def gates(i, _):
        start = pl.multiple_of(i * chunk, chunk)
        s["pre"][pl.ds(start, chunk), :] = jnp.dot(
            s["vb"][pl.ds(start, chunk), :], s["wc"][...], preferred_element_type=f32
        )
        return 0

    lax.fori_loop(0, length // chunk, gates, 0)

    def first(i, carry):
        p0, s0, w0, p1, s1, w1 = carry
        for u in range(0, UNROLL, 2):
            base = i * UNROLL + u
            start = pl.multiple_of(base * SEG, 2 * SEG)
            v_pair = s["vb"][pl.ds(start, 2 * SEG), :].astype(f32)
            for w in range(2):
                r = base + w
                row = pl.multiple_of(r * SEG, SEG)
                v = v_pair[w * SEG : (w + 1) * SEG]
                c = s["cp"][r]
                spike = s["spk"][r]
                found = []
                for d in range(2):
                    th = jnp.tanh(0.5 * s["pre"][pl.ds(row, SEG), 2 * d * LANES : (2 * d + 1) * LANES])
                    tg = jnp.tanh(0.5 * s["pre"][pl.ds(row, SEG), (2 * d + 1) * LANES : (2 * d + 2) * LANES])
                    log_decay = k4[d] * th + (k4[d] + spike)
                    decay = jnp.exp(log_decay)
                    decay2 = decay * decay
                    m2 = -jnp.tanh(log_decay) * (1.0 + decay2)
                    inverse = lax.rsqrt(m2)
                    half = 0.5 * tg
                    gate = 0.5 + half
                    slope = (m2 * inverse) * gate
                    source = slope * v
                    s["dec"][d, r] = decay
                    s["src"][d, r] = source
                    s["slope"][d, r] = slope
                    s["second"][d, r] = gate * v * decay2 * inverse
                    s["rate"][d, r] = k2[d] * (1.0 - th * th)
                    s["gate"][d, r] = source * (0.5 - half)
                    found.append((decay, source))
                (d0, g0), (d1, g1) = found
                s0 = d0 * s0 + g0
                p0 = p0 * d0
                w0 = w0 + p0 * c
                w1 = d1 * (c + w1)
                s1 = s1 + p1 * g1
                p1 = p1 * d1
        return p0, s0, w0, p1, s1, w1

    zero = jnp.zeros(tile, f32)
    one = jnp.ones(tile, f32)
    p0, s0, w0, p1, s1, w1 = lax.fori_loop(0, rows // UNROLL, first, (one, zero, zero, one, zero, zero))
    s0 = carry_in(p0, s0, True)
    w0 = carry_in(p0, w0, False)
    w1 = carry_in(p1, w1, True)
    s1 = carry_in(p1, s1, False)

    def forward(i, carry):
        state, back = carry
        for u in range(UNROLL):
            r = i * UNROLL + u
            moved = s["dec"][0, r] * state
            state = moved + s["src"][0, r]
            s["rate"][0, r] = (moved - s["second"][0, r]) * s["rate"][0, r]
            adjoint = s["cp"][r] + back
            back = s["dec"][1, r] * adjoint
            s["adj"][r] = adjoint
        return state, back

    lax.fori_loop(0, rows // UNROLL, forward, (s0, w1))

    def reverse(i, carry):
        state, back = carry
        for u in range(UNROLL - 2, -2, -2):
            base = rows - (i + 1) * UNROLL + u
            parts = [None, None]
            for w in (1, 0):
                r = base + w
                adjoint = s["cp"][r] + back
                back = s["dec"][0, r] * adjoint
                moved = s["dec"][1, r] * state
                state = moved + s["src"][1, r]
                other = s["adj"][r]
                s["vg"][r + 1] = adjoint * s["slope"][0, r] + other * s["slope"][1, r]
                parts[w] = (
                    adjoint * s["rate"][0, r],
                    adjoint * s["gate"][0, r],
                    other * ((moved - s["second"][1, r]) * s["rate"][1, r]),
                    other * s["gate"][1, r],
                )
            start = pl.multiple_of(base * SEG, 2 * SEG)
            for j in range(4):
                s["back"][pl.ds(start, 2 * SEG), j * LANES : (j + 1) * LANES] = jnp.concatenate(
                    [parts[0][j], parts[1][j]], axis=0
                ).astype(bf16)
        return state, back

    lax.fori_loop(0, rows // UNROLL, reverse, (s1, w0))

    vg = s["vg"]

    def through(i, _):
        start = pl.multiple_of(i * chunk, chunk)
        part = lax.dot_general(
            s["back"][pl.ds(start, chunk), :],
            s["wc"][...],
            (((1,), (1,)), ((), ())),
            preferred_element_type=f32,
        )
        where = pl.ds(i * (chunk // SEG) + 1, chunk // SEG)
        vg[where] = vg[where] + part.reshape(chunk // SEG, SEG, LANES)
        return 0

    lax.fori_loop(0, length // chunk, through, 0)
    vg[0] = shift_segments(vg[rows], True)
    vg[rows + 1] = shift_segments(vg[1], False)
    vg[rows + 2] = shift_segments(vg[2], False)

    maps = lax.dot_general(
        s["vb"][...], s["back"][...], (((0,), (0,)), ((), ())), preferred_element_type=f32
    )

    def last(i, sums):
        sums = list(sums)
        for u in range(UNROLL):
            r = i * UNROLL + u
            here = vg[r + 1]
            acc = vg[r + 3] * tap[0] + vg[r + 2] * tap[1] + here * tap[2] + vg[r] * tap[3]
            s["xs"][pl.ds(r, SEG, stride=pitch), :] = acc
            for k in range(4):
                sums[k] = sums[k] + xp[r + k] * here
        return tuple(sums)

    sums = lax.fori_loop(0, rows // UNROLL, last, (zero,) * 4)
    for seg in range(SEG):
        out_gi(seg, s["xs"][pl.ds(seg * pitch, rows), :].astype(bf16))
    tap_rows = jnp.concatenate([jnp.sum(a, axis=0, keepdims=True) for a in sums], axis=0)
    return maps, tap_rows


def head_scratch(rows):
    f32, bf16 = jnp.float32, jnp.bfloat16
    length = rows * SEG
    pitch = rows + SEG
    per = lambda n: pltpu.VMEM((n, SEG, LANES), f32)
    both = lambda: pltpu.VMEM((2, rows, SEG, LANES), f32)
    return dict(
        xs=pltpu.VMEM((SEG * pitch, LANES), f32),
        cs=pltpu.VMEM((SEG * pitch, LANES), f32),
        ss=pltpu.VMEM((SEG * pitch, LANES), f32),
        xp=per(rows + 3),
        cp=per(rows),
        spk=per(rows),
        vb=pltpu.VMEM((length, LANES), bf16),
        wc=pltpu.VMEM((LANES, 4 * LANES), bf16),
        pre=pltpu.VMEM((length, 4 * LANES), f32),
        dec=both(),
        src=both(),
        slope=both(),
        second=both(),
        rate=both(),
        gate=both(),
        adj=per(rows),
        vg=per(rows + 3),
        back=pltpu.VMEM((length, 4 * LANES), bf16),
    )


def whole_kernel(sizes, norm, x_ref, c_ref, taps_ref, rmap_ref, imap_ref, keep_ref, spike_ref,
                 out_ref, grate_ref, ginput_ref, gtaps_ref, s):
    n, m, heads, tok, rows, q = sizes
    f32, bf16 = jnp.float32, jnp.bfloat16
    me = lax.axis_index("sp")
    mine = lax.axis_index("dp")
    cols = heads * LANES
    inputs = (x_ref, c_ref)
    wire = s["wbuf"].dtype

    barrier = pltpu.get_barrier_semaphore()

    def greet_sp(o, _):
        pl.semaphore_signal(barrier, inc=1, device_id={"sp": lax.rem(me + o, n)},
                            device_id_type=pl.DeviceIdType.MESH)
        return 0

    def greet_dp(o, _):
        pl.semaphore_signal(barrier, inc=1, device_id={"dp": lax.rem(mine + o, m)},
                            device_id_type=pl.DeviceIdType.MESH)
        return 0

    lax.fori_loop(1, n, greet_sp, 0)
    lax.fori_loop(1, m, greet_dp, 0)
    pl.semaphore_wait(barrier, n + m - 2)

    def lanes_of(device, h):
        return pl.ds(pl.multiple_of(device * cols + h * LANES, LANES), LANES)

    def tokens_of(device):
        return pl.ds(pl.multiple_of(device * tok, tok), tok)

    def part_of(device):
        return pl.ds(pl.multiple_of(device * q, q), q)

    def in_copy(a, h, o):
        peer = lax.rem(me + o, n)
        return pltpu.make_async_remote_copy(
            src_ref=inputs[a].at[0, :, lanes_of(peer, h)],
            dst_ref=s["xin"].at[a, h, tokens_of(me), :],
            send_sem=s["in_send"].at[a, h, o - 1],
            recv_sem=s["in_recv"].at[a, h, o - 1],
            device_id={"sp": peer},
            device_id_type=pl.DeviceIdType.MESH,
        )

    def out_copy(h, o):
        peer = lax.rem(me + o, n)
        return pltpu.make_async_remote_copy(
            src_ref=s["gout"].at[h, tokens_of(peer), :],
            dst_ref=out_ref.at[0, :, lanes_of(me, h)],
            send_sem=s["out_send"].at[h, o - 1],
            recv_sem=s["out_recv"].at[h, o - 1],
            device_id={"sp": peer},
            device_id_type=pl.DeviceIdType.MESH,
        )

    def rs_copy(h, o):
        peer = lax.rem(mine + o, m)
        return pltpu.make_async_remote_copy(
            src_ref=s["wbuf"].at[h, part_of(peer), :],
            dst_ref=s["rbuf"].at[h, o - 1],
            send_sem=s["rs_send"].at[h, o - 1],
            recv_sem=s["rs_recv"].at[h, o - 1],
            device_id={"dp": peer},
            device_id_type=pl.DeviceIdType.MESH,
        )

    def ag_copy(h, o):
        peer = lax.rem(mine + o, m)
        return pltpu.make_async_remote_copy(
            src_ref=s["gbuf"].at[h, part_of(mine), :],
            dst_ref=s["gbuf"].at[h, part_of(mine), :],
            send_sem=s["ag_send"].at[h, o - 1],
            recv_sem=s["ag_recv"].at[h, o - 1],
            device_id={"dp": peer},
            device_id_type=pl.DeviceIdType.MESH,
        )

    def tap_copy(o):
        peer = lax.rem(mine + o, m)
        return pltpu.make_async_remote_copy(
            src_ref=s["tbuf"].at[mine],
            dst_ref=s["tbuf"].at[mine],
            send_sem=s["tap_send"].at[o - 1],
            recv_sem=s["tap_recv"].at[o - 1],
            device_id={"dp": peer},
            device_id_type=pl.DeviceIdType.MESH,
        )

    def each(count, act):
        def step(o, _):
            act(o)
            return 0

        lax.fori_loop(1, count, step, 0)

    for h in range(heads):
        for a in range(2):
            each(n, lambda o: in_copy(a, h, o).start())
    for h in range(heads):
        for a in range(2):
            s["xin"][a, h, tokens_of(me), :] = inputs[a][0, :, lanes_of(me, h)]

    def finish_rs(h):
        each(m, lambda o: rs_copy(h, o).wait_recv())

        def add(o, total):
            return total + s["rbuf"][h, o - 1].astype(f32)

        total = lax.fori_loop(1, m, add, s["wbuf"][h, part_of(mine), :].astype(f32))
        s["gbuf"][h, part_of(mine), :] = (total * norm).astype(wire)
        each(m, lambda o: ag_copy(h, o).start())

    def one_head(h, _):
        for a in range(2):
            each(n, lambda o: in_copy(a, h, o).wait_recv())
        load_head(s["xin"].at[0, h], s["xin"].at[1, h], s, rows)
        here = pl.ds(pl.multiple_of(h * LANES, LANES), LANES)

        def out_gi(seg, value):
            s["gout"][h, pl.ds(seg * rows, rows), :] = value

        weights = [
            lambda: rmap_ref[0, h], lambda: imap_ref[0, h],
            lambda: rmap_ref[1, h], lambda: imap_ref[1, h],
        ]
        maps, tap_rows = head_compute(
            s, rows,
            lambda b: s["spike"][h, b : b + 1, :],
            taps_ref[:, here].astype(f32), keep_ref[:, here], weights, out_gi,
        )
        for j in range(4):
            s["wbuf"][h, j * LANES : (j + 1) * LANES, :] = maps[:, j * LANES : (j + 1) * LANES].astype(wire)
        s["tbuf"][mine, h, 0:4, :] = tap_rows * norm
        each(n, lambda o: out_copy(h, o).start())
        each(m, lambda o: rs_copy(h, o).start())
        out_ref[0, :, lanes_of(me, h)] = s["gout"][h, tokens_of(me), :]

        @pl.when(h > 0)
        def _():
            finish_rs(h - 1)

        return 0

    s["tbuf"][mine] = jnp.zeros(s["tbuf"].shape[1:], f32)
    for h in range(heads):
        for b in range(rows * SEG // LANES):
            s["spike"][h, b : b + 1, :] = spike_ref[0, h : h + 1, b * LANES : (b + 1) * LANES]
    lax.fori_loop(0, heads, one_head, 0)
    each(m, lambda o: tap_copy(o).start())
    finish_rs(heads - 1)
    each(m, lambda o: tap_copy(o).wait_recv())

    def add_taps(i, total):
        return total + s["tbuf"][i]

    sums = lax.fori_loop(1, m, add_taps, s["tbuf"][0])
    for h in range(heads):
        gtaps_ref[:, h * LANES : (h + 1) * LANES] = sums[h, 0:4, :]
    for h in range(heads):
        each(m, lambda o: ag_copy(h, o).wait_recv())
        for d in range(2):
            grate_ref[d, h] = s["gbuf"][h, 2 * d * LANES : (2 * d + 1) * LANES, :].astype(f32)
            ginput_ref[d, h] = s["gbuf"][h, (2 * d + 1) * LANES : (2 * d + 2) * LANES, :].astype(f32)
    for h in range(heads):
        each(n, lambda o: out_copy(h, o).wait_recv())
    for h in range(heads):
        for a in range(2):
            each(n, lambda o: in_copy(a, h, o).wait_send())
        each(n, lambda o: out_copy(h, o).wait_send())
        each(m, lambda o: rs_copy(h, o).wait_send())
        each(m, lambda o: ag_copy(h, o).wait_send())
    each(m, lambda o: tap_copy(o).wait_send())


def body(mixing_input, cotangent, filter_taps, recurrence_gate_map, input_gate_map,
         decay_logit_param, spike_decay):
    f32, bf16 = jnp.float32, jnp.bfloat16
    n, m = lax.axis_size("sp"), lax.axis_size("dp")
    heads = recurrence_gate_map.shape[1]
    tok, width = mixing_input.shape[1:]
    length = tok * n
    rows = length // SEG
    q = 4 * LANES // m
    wire = bf16 if q % 16 == 0 else f32
    norm = 1.0 / math.sqrt(m * length)
    dma = lambda *shape: pltpu.SemaphoreType.DMA(shape)
    scratch = dict(
        head_scratch(rows),
        xin=pltpu.VMEM((2, heads, length, LANES), bf16),
        gout=pltpu.VMEM((heads, length, LANES), bf16),
        wbuf=pltpu.VMEM((heads, 4 * LANES, LANES), wire),
        rbuf=pltpu.VMEM((heads, m - 1, q, LANES), wire),
        gbuf=pltpu.VMEM((heads, 4 * LANES, LANES), wire),
        spike=pltpu.VMEM((heads, length // LANES, LANES), f32),
        tbuf=pltpu.VMEM((m, heads, SEG, LANES), f32),
        in_send=dma(2, heads, n - 1),
        in_recv=dma(2, heads, n - 1),
        out_send=dma(heads, n - 1),
        out_recv=dma(heads, n - 1),
        rs_send=dma(heads, m - 1),
        rs_recv=dma(heads, m - 1),
        ag_send=dma(heads, m - 1),
        ag_recv=dma(heads, m - 1),
        tap_send=dma(m - 1),
        tap_recv=dma(m - 1),
    )
    vmem = pl.BlockSpec(memory_space=pltpu.VMEM)
    return pl.pallas_call(
        functools.partial(whole_kernel, (n, m, heads, tok, rows, q), norm),
        in_specs=[vmem] * 7,
        out_specs=[vmem] * 4,
        out_shape=[
            jax.ShapeDtypeStruct(mixing_input.shape, bf16),
            jax.ShapeDtypeStruct(recurrence_gate_map.shape, f32),
            jax.ShapeDtypeStruct(recurrence_gate_map.shape, f32),
            jax.ShapeDtypeStruct((4, heads * LANES), f32),
        ],
        scratch_shapes=[scratch],
        compiler_params=pltpu.CompilerParams(
            collective_id=0, has_side_effects=True, vmem_limit_bytes=56 * 1024 * 1024
        ),
        name="heads_and_exchange",
    )(mixing_input, cotangent, filter_taps, recurrence_gate_map, input_gate_map,
      decay_logit_param, spike_decay)


def solution(mesh):
    return jax.shard_map(
        body,
        mesh=mesh,
        in_specs=(
            P("dp", "sp", None),
            P("dp", "sp", None),
            P(None, "sp"),
            P(None, "sp", None, None),
            P(None, "sp", None, None),
            P(None, "sp"),
            P("dp", "sp", None),
        ),
        out_specs=(
            P("dp", "sp", None),
            P(None, "sp", None, None),
            P(None, "sp", None, None),
            P(None, "sp"),
        ),
        check_vma=False,
    )
```

```python
import functools
import math

import jax
import jax.numpy as jnp
from jax import lax
from jax.experimental import pallas as pl
from jax.experimental.pallas import tpu as pltpu
from jax.sharding import PartitionSpec as P

SEG = 8
LANES = 128
UNROLL = 4


def shift_segments(rows, down):
    index = lax.broadcasted_iota(jnp.int32, rows.shape, 0)
    if down:
        return jnp.where(index == 0, 0.0, pltpu.roll(rows, 1, 0))
    return jnp.where(index == SEG - 1, 0.0, pltpu.roll(rows, SEG - 1, 0))


def carry_in(product, total, down):
    p = shift_segments(product, down)
    q = shift_segments(total, down)
    for step in (1, 2, 4):
        amount = step if down else SEG - step
        q = q + p * pltpu.roll(q, amount, 0)
        p = p * pltpu.roll(p, amount, 0)
    return q


def load_head(x_ref, c_ref, s, rows):
    pitch = rows + SEG
    for seg in range(SEG):
        s["xs"][pl.ds(seg * pitch, rows), :] = x_ref[pl.ds(seg * rows, rows), :].astype(jnp.float32)
        s["cs"][pl.ds(seg * pitch, rows), :] = c_ref[pl.ds(seg * rows, rows), :].astype(jnp.float32)


def head_compute(s, rows, spike_row, taps, keep, weights, out_gi):
    f32, bf16 = jnp.float32, jnp.bfloat16
    pitch = rows + SEG
    length = rows * SEG
    tile = (SEG, LANES)
    tap = [jnp.broadcast_to(taps[k : k + 1, :], tile) for k in range(4)]
    logit = keep
    log_keep = jnp.minimum(logit, 0.0) - jnp.log1p(jnp.exp(-jnp.abs(logit)))
    k4 = [jnp.broadcast_to(4.0 * log_keep[d : d + 1, :], tile) for d in range(2)]
    k2 = [jnp.broadcast_to(2.0 * log_keep[d : d + 1, :], tile) for d in range(2)]

    for j in range(4):
        s["wc"][:, j * LANES : (j + 1) * LANES] = weights[j]()
    piece = min(rows, LANES)
    for b in range(length // LANES):
        block = jnp.transpose(
            jnp.broadcast_to(spike_row(b), (LANES, LANES))
        )
        for e in range(LANES // piece):
            at = b * LANES + e * piece
            where = at // rows * pitch + at % rows
            s["ss"][pl.ds(where, piece), :] = block[e * piece : (e + 1) * piece]

    def permute(i, _):
        for u in range(UNROLL):
            r = i * UNROLL + u
            s["xp"][r + 2] = s["xs"][pl.ds(r, SEG, stride=pitch), :]
            s["cp"][r] = s["cs"][pl.ds(r, SEG, stride=pitch), :]
            s["spk"][r] = s["ss"][pl.ds(r, SEG, stride=pitch), :]
        return 0

    lax.fori_loop(0, rows // UNROLL, permute, 0)
    xp = s["xp"]
    xp[0] = shift_segments(xp[rows], True)
    xp[1] = shift_segments(xp[rows + 1], True)
    xp[rows + 2] = shift_segments(xp[2], False)

    def conv(i, _):
        for u in range(0, UNROLL, 2):
            r = i * UNROLL + u
            pair = []
            for w in range(2):
                acc = xp[r + w] * tap[0]
                for k in range(1, 4):
                    acc = acc + xp[r + w + k] * tap[k]
                pair.append(acc)
            start = pl.multiple_of(r * SEG, 2 * SEG)
            s["vb"][pl.ds(start, 2 * SEG), :] = jnp.concatenate(pair, axis=0).astype(bf16)
        return 0

    lax.fori_loop(0, rows // UNROLL, conv, 0)

    chunk = 256

    def gates(i, _):
        start = pl.multiple_of(i * chunk, chunk)
        s["pre"][pl.ds(start, chunk), :] = jnp.dot(
            s["vb"][pl.ds(start, chunk), :], s["wc"][...], preferred_element_type=f32
        )
        return 0

    lax.fori_loop(0, length // chunk, gates, 0)

    def first(i, carry):
        p0, s0, w0, p1, s1, w1 = carry
        for u in range(0, UNROLL, 2):
            base = i * UNROLL + u
            start = pl.multiple_of(base * SEG, 2 * SEG)
            v_pair = s["vb"][pl.ds(start, 2 * SEG), :].astype(f32)
            for w in range(2):
                r = base + w
                row = pl.multiple_of(r * SEG, SEG)
                v = v_pair[w * SEG : (w + 1) * SEG]
                c = s["cp"][r]
                spike = s["spk"][r]
                found = []
                for d in range(2):
                    th = jnp.tanh(0.5 * s["pre"][pl.ds(row, SEG), 2 * d * LANES : (2 * d + 1) * LANES])
                    tg = jnp.tanh(0.5 * s["pre"][pl.ds(row, SEG), (2 * d + 1) * LANES : (2 * d + 2) * LANES])
                    log_decay = k4[d] * th + (k4[d] + spike)
                    decay = jnp.exp(log_decay)
                    decay2 = decay * decay
                    m2 = -jnp.tanh(log_decay) * (1.0 + decay2)
                    inverse = lax.rsqrt(m2)
                    half = 0.5 * tg
                    gate = 0.5 + half
                    slope = (m2 * inverse) * gate
                    source = slope * v
                    s["dec"][d, r] = decay
                    s["src"][d, r] = source
                    s["slope"][d, r] = slope
                    s["second"][d, r] = gate * v * decay2 * inverse
                    s["rate"][d, r] = k2[d] * (1.0 - th * th)
                    s["gate"][d, r] = source * (0.5 - half)
                    found.append((decay, source))
                (d0, g0), (d1, g1) = found
                s0 = d0 * s0 + g0
                p0 = p0 * d0
                w0 = w0 + p0 * c
                w1 = d1 * (c + w1)
                s1 = s1 + p1 * g1
                p1 = p1 * d1
        return p0, s0, w0, p1, s1, w1

    zero = jnp.zeros(tile, f32)
    one = jnp.ones(tile, f32)
    p0, s0, w0, p1, s1, w1 = lax.fori_loop(0, rows // UNROLL, first, (one, zero, zero, one, zero, zero))
    s0 = carry_in(p0, s0, True)
    w0 = carry_in(p0, w0, False)
    w1 = carry_in(p1, w1, True)
    s1 = carry_in(p1, s1, False)

    def forward(i, carry):
        state, back = carry
        for u in range(UNROLL):
            r = i * UNROLL + u
            moved = s["dec"][0, r] * state
            state = moved + s["src"][0, r]
            s["rate"][0, r] = (moved - s["second"][0, r]) * s["rate"][0, r]
            adjoint = s["cp"][r] + back
            back = s["dec"][1, r] * adjoint
            s["adj"][r] = adjoint
        return state, back

    lax.fori_loop(0, rows // UNROLL, forward, (s0, w1))

    def reverse(i, carry):
        state, back = carry
        for u in range(UNROLL - 2, -2, -2):
            base = rows - (i + 1) * UNROLL + u
            parts = [None, None]
            for w in (1, 0):
                r = base + w
                adjoint = s["cp"][r] + back
                back = s["dec"][0, r] * adjoint
                moved = s["dec"][1, r] * state
                state = moved + s["src"][1, r]
                other = s["adj"][r]
                s["vg"][r + 1] = adjoint * s["slope"][0, r] + other * s["slope"][1, r]
                parts[w] = (
                    adjoint * s["rate"][0, r],
                    adjoint * s["gate"][0, r],
                    other * ((moved - s["second"][1, r]) * s["rate"][1, r]),
                    other * s["gate"][1, r],
                )
            start = pl.multiple_of(base * SEG, 2 * SEG)
            for j in range(4):
                s["back"][pl.ds(start, 2 * SEG), j * LANES : (j + 1) * LANES] = jnp.concatenate(
                    [parts[0][j], parts[1][j]], axis=0
                ).astype(bf16)
        return state, back

    lax.fori_loop(0, rows // UNROLL, reverse, (s1, w0))

    vg = s["vg"]

    def through(i, _):
        start = pl.multiple_of(i * chunk, chunk)
        part = lax.dot_general(
            s["back"][pl.ds(start, chunk), :],
            s["wc"][...],
            (((1,), (1,)), ((), ())),
            preferred_element_type=f32,
        )
        where = pl.ds(i * (chunk // SEG) + 1, chunk // SEG)
        vg[where] = vg[where] + part.reshape(chunk // SEG, SEG, LANES)
        return 0

    lax.fori_loop(0, length // chunk, through, 0)
    vg[0] = shift_segments(vg[rows], True)
    vg[rows + 1] = shift_segments(vg[1], False)
    vg[rows + 2] = shift_segments(vg[2], False)

    maps = lax.dot_general(
        s["vb"][...], s["back"][...], (((0,), (0,)), ((), ())), preferred_element_type=f32
    )

    def last(i, sums):
        sums = list(sums)
        for u in range(UNROLL):
            r = i * UNROLL + u
            here = vg[r + 1]
            acc = vg[r + 3] * tap[0] + vg[r + 2] * tap[1] + here * tap[2] + vg[r] * tap[3]
            s["xs"][pl.ds(r, SEG, stride=pitch), :] = acc
            for k in range(4):
                sums[k] = sums[k] + xp[r + k] * here
        return tuple(sums)

    sums = lax.fori_loop(0, rows // UNROLL, last, (zero,) * 4)
    for seg in range(SEG):
        out_gi(seg, s["xs"][pl.ds(seg * pitch, rows), :].astype(bf16))
    tap_rows = jnp.concatenate([jnp.sum(a, axis=0, keepdims=True) for a in sums], axis=0)
    return maps, tap_rows


def head_scratch(rows):
    f32, bf16 = jnp.float32, jnp.bfloat16
    length = rows * SEG
    pitch = rows + SEG
    per = lambda n: pltpu.VMEM((n, SEG, LANES), f32)
    both = lambda: pltpu.VMEM((2, rows, SEG, LANES), f32)
    return dict(
        xs=pltpu.VMEM((SEG * pitch, LANES), f32),
        cs=pltpu.VMEM((SEG * pitch, LANES), f32),
        ss=pltpu.VMEM((SEG * pitch, LANES), f32),
        xp=per(rows + 3),
        cp=per(rows),
        spk=per(rows),
        vb=pltpu.VMEM((length, LANES), bf16),
        wc=pltpu.VMEM((LANES, 4 * LANES), bf16),
        pre=pltpu.VMEM((length, 4 * LANES), f32),
        dec=both(),
        src=both(),
        slope=both(),
        second=both(),
        rate=both(),
        gate=both(),
        adj=per(rows),
        vg=per(rows + 3),
        back=pltpu.VMEM((length, 4 * LANES), bf16),
    )


def whole_kernel(sizes, norm, x_ref, c_ref, taps_hbm, rmap_hbm, imap_hbm, keep_hbm, spike_hbm,
                 out_ref, maps_ref, tap_ref, s):
    n, m, heads, tok, rows, q = sizes
    f32, bf16 = jnp.float32, jnp.bfloat16
    me = lax.axis_index("sp")
    mine = lax.axis_index("dp")
    cols = heads * LANES
    inputs = (x_ref, c_ref)
    wire = s["wbuf"].dtype

    taps_ref, rmap_ref, imap_ref, keep_ref, spike_ref = s["small"]
    small = [
        pltpu.make_async_copy(source, target, s["small_sem"].at[i])
        for i, (source, target) in enumerate(
            zip((taps_hbm, rmap_hbm, imap_hbm, keep_hbm, spike_hbm), s["small"])
        )
    ]
    for copy in small:
        copy.start()

    barrier = pltpu.get_barrier_semaphore()

    def greet_sp(o, _):
        pl.semaphore_signal(barrier, inc=1, device_id={"sp": lax.rem(me + o, n)},
                            device_id_type=pl.DeviceIdType.MESH)
        return 0

    def greet_dp(o, _):
        pl.semaphore_signal(barrier, inc=1, device_id={"dp": lax.rem(mine + o, m)},
                            device_id_type=pl.DeviceIdType.MESH)
        return 0

    lax.fori_loop(1, n, greet_sp, 0)
    lax.fori_loop(1, m, greet_dp, 0)
    pl.semaphore_wait(barrier, n + m - 2)

    def lanes_of(device, h):
        return pl.ds(pl.multiple_of(device * cols + h * LANES, LANES), LANES)

    def tokens_of(device):
        return pl.ds(pl.multiple_of(device * tok, tok), tok)

    def part_of(device):
        return pl.ds(pl.multiple_of(device * q, q), q)

    def in_copy(a, h, o):
        peer = lax.rem(me + o, n)
        return pltpu.make_async_remote_copy(
            src_ref=inputs[a].at[0, :, lanes_of(peer, h)],
            dst_ref=s["xin"].at[a, h, tokens_of(me), :],
            send_sem=s["in_send"].at[a, h, o - 1],
            recv_sem=s["in_recv"].at[a, h, o - 1],
            device_id={"sp": peer},
            device_id_type=pl.DeviceIdType.MESH,
        )

    def out_copy(h, o):
        peer = lax.rem(me + o, n)
        return pltpu.make_async_remote_copy(
            src_ref=s["gout"].at[h, tokens_of(peer), :],
            dst_ref=out_ref.at[0, :, lanes_of(me, h)],
            send_sem=s["out_send"].at[h, o - 1],
            recv_sem=s["out_recv"].at[h, o - 1],
            device_id={"sp": peer},
            device_id_type=pl.DeviceIdType.MESH,
        )

    def own_in(a, h):
        return pltpu.make_async_copy(
            inputs[a].at[0, :, lanes_of(me, h)], s["xin"].at[a, h, tokens_of(me), :], s["own_in"].at[a, h]
        )

    def own_out(h):
        return pltpu.make_async_copy(
            s["gout"].at[h, tokens_of(me), :], out_ref.at[0, :, lanes_of(me, h)], s["own_out"].at[h]
        )

    def maps_out(h):
        return pltpu.make_async_copy(s["gbuf"].at[h], maps_ref.at[h], s["maps_out"].at[h])

    def rs_copy(h, o):
        peer = lax.rem(mine + o, m)
        return pltpu.make_async_remote_copy(
            src_ref=s["wbuf"].at[h, part_of(peer), :],
            dst_ref=s["rbuf"].at[h, o - 1],
            send_sem=s["rs_send"].at[h, o - 1],
            recv_sem=s["rs_recv"].at[h, o - 1],
            device_id={"dp": peer},
            device_id_type=pl.DeviceIdType.MESH,
        )

    def ag_copy(h, o):
        peer = lax.rem(mine + o, m)
        return pltpu.make_async_remote_copy(
            src_ref=s["gbuf"].at[h, part_of(mine), :],
            dst_ref=s["gbuf"].at[h, part_of(mine), :],
            send_sem=s["ag_send"].at[h, o - 1],
            recv_sem=s["ag_recv"].at[h, o - 1],
            device_id={"dp": peer},
            device_id_type=pl.DeviceIdType.MESH,
        )

    def tap_copy(o):
        peer = lax.rem(mine + o, m)
        return pltpu.make_async_remote_copy(
            src_ref=s["tbuf"].at[mine],
            dst_ref=s["tbuf"].at[mine],
            send_sem=s["tap_send"].at[o - 1],
            recv_sem=s["tap_recv"].at[o - 1],
            device_id={"dp": peer},
            device_id_type=pl.DeviceIdType.MESH,
        )

    def each(count, act):
        def step(o, _):
            act(o)
            return 0

        lax.fori_loop(1, count, step, 0)

    for h in range(heads):
        for a in range(2):
            each(n, lambda o: in_copy(a, h, o).start())
    for h in range(heads):
        for a in range(2):
            own_in(a, h).start()
    for copy in small:
        copy.wait()

    def finish_rs(h):
        each(m, lambda o: rs_copy(h, o).wait_recv())

        def add(o, total):
            return total + s["rbuf"][h, o - 1].astype(f32)

        total = lax.fori_loop(1, m, add, s["wbuf"][h, part_of(mine), :].astype(f32))
        s["gbuf"][h, part_of(mine), :] = (total * norm).astype(wire)
        each(m, lambda o: ag_copy(h, o).start())

    def one_head(h, _):
        for a in range(2):
            own_in(a, h).wait()
            each(n, lambda o: in_copy(a, h, o).wait_recv())
        load_head(s["xin"].at[0, h], s["xin"].at[1, h], s, rows)
        here = pl.ds(pl.multiple_of(h * LANES, LANES), LANES)

        def out_gi(seg, value):
            s["gout"][h, pl.ds(seg * rows, rows), :] = value

        weights = [
            lambda: rmap_ref[0, h], lambda: imap_ref[0, h],
            lambda: rmap_ref[1, h], lambda: imap_ref[1, h],
        ]
        maps, tap_rows = head_compute(
            s, rows,
            lambda b: s["spike"][h, b : b + 1, :],
            taps_ref[:, here].astype(f32), keep_ref[:, here], weights, out_gi,
        )
        for j in range(4):
            s["wbuf"][h, j * LANES : (j + 1) * LANES, :] = maps[:, j * LANES : (j + 1) * LANES].astype(wire)
        s["tbuf"][mine, h, 0:4, :] = tap_rows * norm
        each(n, lambda o: out_copy(h, o).start())
        each(m, lambda o: rs_copy(h, o).start())
        own_out(h).start()

        @pl.when(h > 0)
        def _():
            finish_rs(h - 1)

        return 0

    s["tbuf"][mine] = jnp.zeros(s["tbuf"].shape[1:], f32)
    for h in range(heads):
        for b in range(rows * SEG // LANES):
            s["spike"][h, b : b + 1, :] = spike_ref[0, h : h + 1, b * LANES : (b + 1) * LANES]
    lax.fori_loop(0, heads, one_head, 0)
    each(m, lambda o: tap_copy(o).start())
    finish_rs(heads - 1)
    each(m, lambda o: tap_copy(o).wait_recv())

    def add_taps(i, total):
        return total + s["tbuf"][i]

    s["tsum"][...] = lax.fori_loop(1, m, add_taps, s["tbuf"][0])
    tap_out = pltpu.make_async_copy(s["tsum"], tap_ref, s["small_sem"].at[0])
    tap_out.start()
    for h in range(heads):
        each(m, lambda o: ag_copy(h, o).wait_recv())
        maps_out(h).start()
    for h in range(heads):
        each(n, lambda o: out_copy(h, o).wait_recv())
    for h in range(heads):
        for a in range(2):
            each(n, lambda o: in_copy(a, h, o).wait_send())
        each(n, lambda o: out_copy(h, o).wait_send())
        each(m, lambda o: rs_copy(h, o).wait_send())
        each(m, lambda o: ag_copy(h, o).wait_send())
        own_out(h).wait()
        maps_out(h).wait()
    each(m, lambda o: tap_copy(o).wait_send())
    tap_out.wait()


def finish_kernel(heads, in_ref, maps_ref, tap_ref, out_ref, grate_ref, ginput_ref, gtaps_ref,
                  whole, maps, taps, grate, ginput, gtaps, sem):
    loads = [
        pltpu.make_async_copy(maps_ref, maps, sem.at[0]),
        pltpu.make_async_copy(in_ref, whole, sem.at[1]),
        pltpu.make_async_copy(tap_ref, taps, sem.at[2]),
    ]
    stores = [
        pltpu.make_async_copy(grate, grate_ref, sem.at[3]),
        pltpu.make_async_copy(ginput, ginput_ref, sem.at[4]),
        pltpu.make_async_copy(whole, out_ref, sem.at[5]),
        pltpu.make_async_copy(gtaps, gtaps_ref, sem.at[6]),
    ]
    for copy in loads:
        copy.start()
    loads[0].wait()
    loads[1].wait()
    stores[2].start()
    for i, target in enumerate((grate, ginput)):
        for h in range(heads):
            for d in range(2):
                j = 2 * d + i
                target[d, h] = maps[h, j * LANES : (j + 1) * LANES, :].astype(jnp.float32)
        stores[i].start()
    loads[2].wait()
    for h in range(heads):
        gtaps[:, h * LANES : (h + 1) * LANES] = taps[h, 0:4, :]
    stores[3].start()
    for copy in stores:
        copy.wait()


def body(mixing_input, cotangent, filter_taps, recurrence_gate_map, input_gate_map,
         decay_logit_param, spike_decay):
    f32, bf16 = jnp.float32, jnp.bfloat16
    n, m = lax.axis_size("sp"), lax.axis_size("dp")
    heads = recurrence_gate_map.shape[1]
    tok, width = mixing_input.shape[1:]
    length = tok * n
    rows = length // SEG
    q = 4 * LANES // m
    wire = bf16 if q % 16 == 0 else f32
    norm = 1.0 / math.sqrt(m * length)
    dma = lambda *shape: pltpu.SemaphoreType.DMA(shape)
    scratch = dict(
        head_scratch(rows),
        xin=pltpu.VMEM((2, heads, length, LANES), bf16),
        gout=pltpu.VMEM((heads, length, LANES), bf16),
        wbuf=pltpu.VMEM((heads, 4 * LANES, LANES), wire),
        rbuf=pltpu.VMEM((heads, m - 1, q, LANES), wire),
        gbuf=pltpu.VMEM((heads, 4 * LANES, LANES), wire),
        spike=pltpu.VMEM((heads, length // LANES, LANES), f32),
        tbuf=pltpu.VMEM((m, heads, SEG, LANES), f32),
        tsum=pltpu.VMEM((heads, SEG, LANES), f32),
        small=tuple(
            pltpu.VMEM(a.shape, a.dtype)
            for a in (filter_taps, recurrence_gate_map, input_gate_map, decay_logit_param, spike_decay)
        ),
        small_sem=dma(5),
        own_in=dma(2, heads),
        own_out=dma(heads),
        maps_out=dma(heads),
        in_send=dma(2, heads, n - 1),
        in_recv=dma(2, heads, n - 1),
        out_send=dma(heads, n - 1),
        out_recv=dma(heads, n - 1),
        rs_send=dma(heads, m - 1),
        rs_recv=dma(heads, m - 1),
        ag_send=dma(heads, m - 1),
        ag_recv=dma(heads, m - 1),
        tap_send=dma(m - 1),
        tap_recv=dma(m - 1),
    )
    anywhere = pl.BlockSpec(memory_space=pl.ANY)
    shape = jax.ShapeDtypeStruct
    whole, maps, sums = pl.pallas_call(
        functools.partial(whole_kernel, (n, m, heads, tok, rows, q), norm),
        in_specs=[anywhere] * 7,
        out_specs=[anywhere] * 3,
        out_shape=[
            shape(mixing_input.shape, bf16),
            shape((heads, 4 * LANES, LANES), wire),
            shape((heads, SEG, LANES), f32),
        ],
        scratch_shapes=[scratch],
        compiler_params=pltpu.CompilerParams(
            collective_id=0, has_side_effects=True, vmem_limit_bytes=56 * 1024 * 1024
        ),
        name="heads_and_exchange",
    )(mixing_input, cotangent, filter_taps, recurrence_gate_map, input_gate_map,
      decay_logit_param, spike_decay)
    outs = [
        shape(mixing_input.shape, bf16),
        shape(recurrence_gate_map.shape, f32),
        shape(recurrence_gate_map.shape, f32),
        shape((4, heads * LANES), f32),
    ]
    room = lambda a: pltpu.VMEM(a.shape, a.dtype)
    return pl.pallas_call(
        functools.partial(finish_kernel, heads),
        in_specs=[anywhere] * 3,
        out_specs=[anywhere] * 4,
        out_shape=outs,
        scratch_shapes=[room(whole), room(maps), room(sums), room(outs[1]), room(outs[2]), room(outs[3]), dma(7)],
        compiler_params=pltpu.CompilerParams(vmem_limit_bytes=56 * 1024 * 1024),
        name="finish",
    )(whole, maps, sums)


def solution(mesh):
    return jax.shard_map(
        body,
        mesh=mesh,
        in_specs=(
            P("dp", "sp", None),
            P("dp", "sp", None),
            P(None, "sp"),
            P(None, "sp", None, None),
            P(None, "sp", None, None),
            P(None, "sp"),
            P("dp", "sp", None),
        ),
        out_specs=(
            P("dp", "sp", None),
            P(None, "sp", None, None),
            P(None, "sp", None, None),
            P(None, "sp"),
        ),
        check_vma=False,
    )
```

```python
import functools
import math

import jax
import jax.numpy as jnp
from jax import lax
from jax.experimental import pallas as pl
from jax.experimental.pallas import tpu as pltpu
from jax.sharding import PartitionSpec as P

SEG = 8
LANES = 128
UNROLL = 4


def shift_segments(rows, down):
    index = lax.broadcasted_iota(jnp.int32, rows.shape, 0)
    if down:
        return jnp.where(index == 0, 0.0, pltpu.roll(rows, 1, 0))
    return jnp.where(index == SEG - 1, 0.0, pltpu.roll(rows, SEG - 1, 0))


def carry_in(product, total, down):
    p = shift_segments(product, down)
    q = shift_segments(total, down)
    for step in (1, 2, 4):
        amount = step if down else SEG - step
        q = q + p * pltpu.roll(q, amount, 0)
        p = p * pltpu.roll(p, amount, 0)
    return q


def load_head(x_ref, c_ref, s, rows):
    pitch = rows + SEG
    for seg in range(SEG):
        s["xs"][pl.ds(seg * pitch, rows), :] = x_ref[pl.ds(seg * rows, rows), :].astype(jnp.float32)
        s["cs"][pl.ds(seg * pitch, rows), :] = c_ref[pl.ds(seg * rows, rows), :].astype(jnp.float32)


def head_compute(s, rows, spike_row, taps, keep, weights, out_gi):
    f32, bf16 = jnp.float32, jnp.bfloat16
    pitch = rows + SEG
    length = rows * SEG
    tile = (SEG, LANES)
    tap = [jnp.broadcast_to(taps[k : k + 1, :], tile) for k in range(4)]
    logit = keep
    log_keep = jnp.minimum(logit, 0.0) - jnp.log1p(jnp.exp(-jnp.abs(logit)))
    k4 = [jnp.broadcast_to(4.0 * log_keep[d : d + 1, :], tile) for d in range(2)]
    k2 = [jnp.broadcast_to(2.0 * log_keep[d : d + 1, :], tile) for d in range(2)]

    for j in range(4):
        s["wc"][:, j * LANES : (j + 1) * LANES] = weights[j]()
    piece = min(rows, LANES)
    for b in range(length // LANES):
        block = jnp.transpose(
            jnp.broadcast_to(spike_row(b), (LANES, LANES))
        )
        for e in range(LANES // piece):
            at = b * LANES + e * piece
            where = at // rows * pitch + at % rows
            s["ss"][pl.ds(where, piece), :] = block[e * piece : (e + 1) * piece]

    def permute(i, _):
        for u in range(UNROLL):
            r = i * UNROLL + u
            s["xp"][r + 2] = s["xs"][pl.ds(r, SEG, stride=pitch), :]
            s["cp"][r] = s["cs"][pl.ds(r, SEG, stride=pitch), :]
            s["spk"][r] = s["ss"][pl.ds(r, SEG, stride=pitch), :]
        return 0

    lax.fori_loop(0, rows // UNROLL, permute, 0)
    xp = s["xp"]
    xp[0] = shift_segments(xp[rows], True)
    xp[1] = shift_segments(xp[rows + 1], True)
    xp[rows + 2] = shift_segments(xp[2], False)

    def conv(i, _):
        for u in range(0, UNROLL, 2):
            r = i * UNROLL + u
            pair = []
            for w in range(2):
                acc = xp[r + w] * tap[0]
                for k in range(1, 4):
                    acc = acc + xp[r + w + k] * tap[k]
                pair.append(acc)
            start = pl.multiple_of(r * SEG, 2 * SEG)
            s["vb"][pl.ds(start, 2 * SEG), :] = jnp.concatenate(pair, axis=0).astype(bf16)
        return 0

    lax.fori_loop(0, rows // UNROLL, conv, 0)

    chunk = 256

    def gates(i, _):
        start = pl.multiple_of(i * chunk, chunk)
        s["pre"][pl.ds(start, chunk), :] = jnp.dot(
            s["vb"][pl.ds(start, chunk), :], s["wc"][...], preferred_element_type=f32
        )
        return 0

    lax.fori_loop(0, length // chunk, gates, 0)

    def first(i, carry):
        p0, s0, w0, p1, s1, w1 = carry
        for u in range(0, UNROLL, 2):
            base = i * UNROLL + u
            start = pl.multiple_of(base * SEG, 2 * SEG)
            v_pair = s["vb"][pl.ds(start, 2 * SEG), :].astype(f32)
            for w in range(2):
                r = base + w
                row = pl.multiple_of(r * SEG, SEG)
                v = v_pair[w * SEG : (w + 1) * SEG]
                c = s["cp"][r]
                spike = s["spk"][r]
                found = []
                for d in range(2):
                    th = jnp.tanh(0.5 * s["pre"][pl.ds(row, SEG), 2 * d * LANES : (2 * d + 1) * LANES])
                    tg = jnp.tanh(0.5 * s["pre"][pl.ds(row, SEG), (2 * d + 1) * LANES : (2 * d + 2) * LANES])
                    log_decay = k4[d] * th + (k4[d] + spike)
                    decay = jnp.exp(log_decay)
                    decay2 = decay * decay
                    m2 = -jnp.tanh(log_decay) * (1.0 + decay2)
                    inverse = lax.rsqrt(m2)
                    half = 0.5 * tg
                    gate = 0.5 + half
                    slope = (m2 * inverse) * gate
                    source = slope * v
                    s["dec"][d, r] = decay
                    s["src"][d, r] = source
                    s["slope"][d, r] = slope
                    s["second"][d, r] = gate * v * decay2 * inverse
                    s["rate"][d, r] = k2[d] * (1.0 - th * th)
                    s["gate"][d, r] = source * (0.5 - half)
                    found.append((decay, source))
                (d0, g0), (d1, g1) = found
                s0 = d0 * s0 + g0
                p0 = p0 * d0
                w0 = w0 + p0 * c
                w1 = d1 * (c + w1)
                s1 = s1 + p1 * g1
                p1 = p1 * d1
        return p0, s0, w0, p1, s1, w1

    zero = jnp.zeros(tile, f32)
    one = jnp.ones(tile, f32)
    p0, s0, w0, p1, s1, w1 = lax.fori_loop(0, rows // UNROLL, first, (one, zero, zero, one, zero, zero))
    s0 = carry_in(p0, s0, True)
    w0 = carry_in(p0, w0, False)
    w1 = carry_in(p1, w1, True)
    s1 = carry_in(p1, s1, False)

    def forward(i, carry):
        state, back = carry
        for u in range(UNROLL):
            r = i * UNROLL + u
            moved = s["dec"][0, r] * state
            state = moved + s["src"][0, r]
            s["rate"][0, r] = (moved - s["second"][0, r]) * s["rate"][0, r]
            adjoint = s["cp"][r] + back
            back = s["dec"][1, r] * adjoint
            s["adj"][r] = adjoint
        return state, back

    lax.fori_loop(0, rows // UNROLL, forward, (s0, w1))

    def reverse(i, carry):
        state, back = carry
        for u in range(UNROLL - 2, -2, -2):
            base = rows - (i + 1) * UNROLL + u
            parts = [None, None]
            for w in (1, 0):
                r = base + w
                adjoint = s["cp"][r] + back
                back = s["dec"][0, r] * adjoint
                moved = s["dec"][1, r] * state
                state = moved + s["src"][1, r]
                other = s["adj"][r]
                s["vg"][r + 1] = adjoint * s["slope"][0, r] + other * s["slope"][1, r]
                parts[w] = (
                    adjoint * s["rate"][0, r],
                    adjoint * s["gate"][0, r],
                    other * ((moved - s["second"][1, r]) * s["rate"][1, r]),
                    other * s["gate"][1, r],
                )
            start = pl.multiple_of(base * SEG, 2 * SEG)
            for j in range(4):
                s["back"][pl.ds(start, 2 * SEG), j * LANES : (j + 1) * LANES] = jnp.concatenate(
                    [parts[0][j], parts[1][j]], axis=0
                ).astype(bf16)
        return state, back

    lax.fori_loop(0, rows // UNROLL, reverse, (s1, w0))

    vg = s["vg"]

    def through(i, _):
        start = pl.multiple_of(i * chunk, chunk)
        part = lax.dot_general(
            s["back"][pl.ds(start, chunk), :],
            s["wc"][...],
            (((1,), (1,)), ((), ())),
            preferred_element_type=f32,
        )
        where = pl.ds(i * (chunk // SEG) + 1, chunk // SEG)
        vg[where] = vg[where] + part.reshape(chunk // SEG, SEG, LANES)
        return 0

    lax.fori_loop(0, length // chunk, through, 0)
    vg[0] = shift_segments(vg[rows], True)
    vg[rows + 1] = shift_segments(vg[1], False)
    vg[rows + 2] = shift_segments(vg[2], False)

    maps = lax.dot_general(
        s["vb"][...], s["back"][...], (((0,), (0,)), ((), ())), preferred_element_type=f32
    )

    def last(i, sums):
        sums = list(sums)
        for u in range(UNROLL):
            r = i * UNROLL + u
            here = vg[r + 1]
            acc = vg[r + 3] * tap[0] + vg[r + 2] * tap[1] + here * tap[2] + vg[r] * tap[3]
            s["xs"][pl.ds(r, SEG, stride=pitch), :] = acc
            for k in range(4):
                sums[k] = sums[k] + xp[r + k] * here
        return tuple(sums)

    sums = lax.fori_loop(0, rows // UNROLL, last, (zero,) * 4)
    for seg in range(SEG):
        out_gi(seg, s["xs"][pl.ds(seg * pitch, rows), :].astype(bf16))
    tap_rows = jnp.concatenate([jnp.sum(a, axis=0, keepdims=True) for a in sums], axis=0)
    return maps, tap_rows


def head_scratch(rows):
    f32, bf16 = jnp.float32, jnp.bfloat16
    length = rows * SEG
    pitch = rows + SEG
    per = lambda n: pltpu.VMEM((n, SEG, LANES), f32)
    both = lambda: pltpu.VMEM((2, rows, SEG, LANES), f32)
    return dict(
        xs=pltpu.VMEM((SEG * pitch, LANES), f32),
        cs=pltpu.VMEM((SEG * pitch, LANES), f32),
        ss=pltpu.VMEM((SEG * pitch, LANES), f32),
        xp=per(rows + 3),
        cp=per(rows),
        spk=per(rows),
        vb=pltpu.VMEM((length, LANES), bf16),
        wc=pltpu.VMEM((LANES, 4 * LANES), bf16),
        pre=pltpu.VMEM((length, 4 * LANES), f32),
        dec=both(),
        src=both(),
        slope=both(),
        second=both(),
        rate=both(),
        gate=both(),
        adj=per(rows),
        vg=per(rows + 3),
        back=pltpu.VMEM((length, 4 * LANES), bf16),
    )


def whole_kernel(sizes, norm, x_ref, c_ref, taps_hbm, rmap_hbm, imap_hbm, keep_hbm, spike_hbm,
                 out_ref, maps_ref, tap_ref, s):
    n, m, heads, tok, rows, q = sizes
    f32, bf16 = jnp.float32, jnp.bfloat16
    me = lax.axis_index("sp")
    mine = lax.axis_index("dp")
    cols = heads * LANES
    inputs = (x_ref, c_ref)
    wire = s["wbuf"].dtype

    taps_ref, rmap_ref, imap_ref, keep_ref, spike_ref = s["small"]
    small = [
        pltpu.make_async_copy(source, target, s["small_sem"].at[i])
        for i, (source, target) in enumerate(
            zip((taps_hbm, rmap_hbm, imap_hbm, keep_hbm, spike_hbm), s["small"])
        )
    ]
    barrier = pltpu.get_barrier_semaphore()

    def greet_sp(o, _):
        pl.semaphore_signal(barrier, inc=1, device_id={"sp": lax.rem(me + o, n)},
                            device_id_type=pl.DeviceIdType.MESH)
        return 0

    def greet_dp(o, _):
        pl.semaphore_signal(barrier, inc=1, device_id={"dp": lax.rem(mine + o, m)},
                            device_id_type=pl.DeviceIdType.MESH)
        return 0

    def lanes_of(device, h):
        return pl.ds(pl.multiple_of(device * cols + h * LANES, LANES), LANES)

    def tokens_of(device):
        return pl.ds(pl.multiple_of(device * tok, tok), tok)

    def own_in(a, h):
        return pltpu.make_async_copy(
            inputs[a].at[0, :, lanes_of(me, h)], s["xin"].at[a, h, tokens_of(me), :], s["own_in"].at[a, h]
        )

    lax.fori_loop(1, n, greet_sp, 0)
    lax.fori_loop(1, m, greet_dp, 0)
    for copy in small:
        copy.start()
    for h in range(heads):
        for a in range(2):
            own_in(a, h).start()
    pl.semaphore_wait(barrier, n + m - 2)

    def part_of(device):
        return pl.ds(pl.multiple_of(device * q, q), q)

    def in_copy(a, h, o):
        peer = lax.rem(me + o, n)
        return pltpu.make_async_remote_copy(
            src_ref=inputs[a].at[0, :, lanes_of(peer, h)],
            dst_ref=s["xin"].at[a, h, tokens_of(me), :],
            send_sem=s["in_send"].at[a, h, o - 1],
            recv_sem=s["in_recv"].at[a, h, o - 1],
            device_id={"sp": peer},
            device_id_type=pl.DeviceIdType.MESH,
        )

    def out_copy(h, o):
        peer = lax.rem(me + o, n)
        return pltpu.make_async_remote_copy(
            src_ref=s["gout"].at[h, tokens_of(peer), :],
            dst_ref=out_ref.at[0, :, lanes_of(me, h)],
            send_sem=s["out_send"].at[h, o - 1],
            recv_sem=s["out_recv"].at[h, o - 1],
            device_id={"sp": peer},
            device_id_type=pl.DeviceIdType.MESH,
        )

    def own_out(h):
        return pltpu.make_async_copy(
            s["gout"].at[h, tokens_of(me), :], out_ref.at[0, :, lanes_of(me, h)], s["own_out"].at[h]
        )

    def maps_out(h):
        return pltpu.make_async_copy(s["gbuf"].at[h], maps_ref.at[h], s["maps_out"].at[h])

    def rs_copy(h, o):
        peer = lax.rem(mine + o, m)
        return pltpu.make_async_remote_copy(
            src_ref=s["wbuf"].at[h, part_of(peer), :],
            dst_ref=s["rbuf"].at[h, o - 1],
            send_sem=s["rs_send"].at[h, o - 1],
            recv_sem=s["rs_recv"].at[h, o - 1],
            device_id={"dp": peer},
            device_id_type=pl.DeviceIdType.MESH,
        )

    def ag_copy(h, o):
        peer = lax.rem(mine + o, m)
        return pltpu.make_async_remote_copy(
            src_ref=s["gbuf"].at[h, part_of(mine), :],
            dst_ref=s["gbuf"].at[h, part_of(mine), :],
            send_sem=s["ag_send"].at[h, o - 1],
            recv_sem=s["ag_recv"].at[h, o - 1],
            device_id={"dp": peer},
            device_id_type=pl.DeviceIdType.MESH,
        )

    def tap_copy(o):
        peer = lax.rem(mine + o, m)
        return pltpu.make_async_remote_copy(
            src_ref=s["tbuf"].at[mine],
            dst_ref=s["tbuf"].at[mine],
            send_sem=s["tap_send"].at[o - 1],
            recv_sem=s["tap_recv"].at[o - 1],
            device_id={"dp": peer},
            device_id_type=pl.DeviceIdType.MESH,
        )

    def each(count, act):
        def step(o, _):
            act(o)
            return 0

        lax.fori_loop(1, count, step, 0)

    for h in range(heads):
        for a in range(2):
            each(n, lambda o: in_copy(a, h, o).start())
    for copy in small:
        copy.wait()

    def finish_rs(h):
        each(m, lambda o: rs_copy(h, o).wait_recv())

        def add(o, total):
            return total + s["rbuf"][h, o - 1].astype(f32)

        total = lax.fori_loop(1, m, add, s["wbuf"][h, part_of(mine), :].astype(f32))
        s["gbuf"][h, part_of(mine), :] = (total * norm).astype(wire)
        each(m, lambda o: ag_copy(h, o).start())

    def one_head(h, _):
        for a in range(2):
            own_in(a, h).wait()
            each(n, lambda o: in_copy(a, h, o).wait_recv())
        load_head(s["xin"].at[0, h], s["xin"].at[1, h], s, rows)
        here = pl.ds(pl.multiple_of(h * LANES, LANES), LANES)

        def out_gi(seg, value):
            s["gout"][h, pl.ds(seg * rows, rows), :] = value

        weights = [
            lambda: rmap_ref[0, h], lambda: imap_ref[0, h],
            lambda: rmap_ref[1, h], lambda: imap_ref[1, h],
        ]
        maps, tap_rows = head_compute(
            s, rows,
            lambda b: s["spike"][h, b : b + 1, :],
            taps_ref[:, here].astype(f32), keep_ref[:, here], weights, out_gi,
        )
        for j in range(4):
            s["wbuf"][h, j * LANES : (j + 1) * LANES, :] = maps[:, j * LANES : (j + 1) * LANES].astype(wire)
        s["tbuf"][mine, h, 0:4, :] = tap_rows * norm
        each(n, lambda o: out_copy(h, o).start())
        each(m, lambda o: rs_copy(h, o).start())
        own_out(h).start()

        @pl.when(h > 0)
        def _():
            finish_rs(h - 1)

        return 0

    s["tbuf"][mine] = jnp.zeros(s["tbuf"].shape[1:], f32)
    for h in range(heads):
        for b in range(rows * SEG // LANES):
            s["spike"][h, b : b + 1, :] = spike_ref[0, h : h + 1, b * LANES : (b + 1) * LANES]
    lax.fori_loop(0, heads, one_head, 0)
    each(m, lambda o: tap_copy(o).start())
    for h in range(heads):
        for a in range(2):
            each(n, lambda o: in_copy(a, h, o).wait_send())
    for h in range(heads - 1):
        each(m, lambda o: rs_copy(h, o).wait_send())
    finish_rs(heads - 1)
    each(m, lambda o: tap_copy(o).wait_recv())

    def add_taps(i, total):
        return total + s["tbuf"][i]

    s["tsum"][...] = lax.fori_loop(1, m, add_taps, s["tbuf"][0])
    tap_out = pltpu.make_async_copy(s["tsum"], tap_ref, s["small_sem"].at[0])
    tap_out.start()
    for h in range(heads):
        each(m, lambda o: ag_copy(h, o).wait_recv())
        maps_out(h).start()
    each(m, lambda o: rs_copy(heads - 1, o).wait_send())
    for h in range(heads):
        each(m, lambda o: ag_copy(h, o).wait_send())
        own_out(h).wait()
    each(m, lambda o: tap_copy(o).wait_send())
    tap_out.wait()
    for h in range(heads):
        each(n, lambda o: out_copy(h, o).wait_recv())
    for h in range(heads):
        each(n, lambda o: out_copy(h, o).wait_send())
        maps_out(h).wait()


def finish_kernel(heads, in_ref, maps_ref, tap_ref, out_ref, grate_ref, ginput_ref, gtaps_ref,
                  whole, maps, taps, grate, ginput, gtaps, sem):
    loads = [
        pltpu.make_async_copy(maps_ref, maps, sem.at[0]),
        pltpu.make_async_copy(in_ref, whole, sem.at[1]),
        pltpu.make_async_copy(tap_ref, taps, sem.at[2]),
    ]
    stores = [
        pltpu.make_async_copy(grate, grate_ref, sem.at[3]),
        pltpu.make_async_copy(ginput, ginput_ref, sem.at[4]),
        pltpu.make_async_copy(whole, out_ref, sem.at[5]),
        pltpu.make_async_copy(gtaps, gtaps_ref, sem.at[6]),
    ]
    for copy in loads:
        copy.start()
    loads[0].wait()
    loads[1].wait()
    stores[2].start()
    for i, target in enumerate((grate, ginput)):
        for h in range(heads):
            for d in range(2):
                j = 2 * d + i
                target[d, h] = maps[h, j * LANES : (j + 1) * LANES, :].astype(jnp.float32)
        stores[i].start()
    loads[2].wait()
    for h in range(heads):
        gtaps[:, h * LANES : (h + 1) * LANES] = taps[h, 0:4, :]
    stores[3].start()
    for copy in stores:
        copy.wait()


def body(mixing_input, cotangent, filter_taps, recurrence_gate_map, input_gate_map,
         decay_logit_param, spike_decay):
    f32, bf16 = jnp.float32, jnp.bfloat16
    n, m = lax.axis_size("sp"), lax.axis_size("dp")
    heads = recurrence_gate_map.shape[1]
    tok, width = mixing_input.shape[1:]
    length = tok * n
    rows = length // SEG
    q = 4 * LANES // m
    wire = bf16 if q % 16 == 0 else f32
    norm = 1.0 / math.sqrt(m * length)
    dma = lambda *shape: pltpu.SemaphoreType.DMA(shape)
    scratch = dict(
        head_scratch(rows),
        xin=pltpu.VMEM((2, heads, length, LANES), bf16),
        gout=pltpu.VMEM((heads, length, LANES), bf16),
        wbuf=pltpu.VMEM((heads, 4 * LANES, LANES), wire),
        rbuf=pltpu.VMEM((heads, m - 1, q, LANES), wire),
        gbuf=pltpu.VMEM((heads, 4 * LANES, LANES), wire),
        spike=pltpu.VMEM((heads, length // LANES, LANES), f32),
        tbuf=pltpu.VMEM((m, heads, SEG, LANES), f32),
        tsum=pltpu.VMEM((heads, SEG, LANES), f32),
        small=tuple(
            pltpu.VMEM(a.shape, a.dtype)
            for a in (filter_taps, recurrence_gate_map, input_gate_map, decay_logit_param, spike_decay)
        ),
        small_sem=dma(5),
        own_in=dma(2, heads),
        own_out=dma(heads),
        maps_out=dma(heads),
        in_send=dma(2, heads, n - 1),
        in_recv=dma(2, heads, n - 1),
        out_send=dma(heads, n - 1),
        out_recv=dma(heads, n - 1),
        rs_send=dma(heads, m - 1),
        rs_recv=dma(heads, m - 1),
        ag_send=dma(heads, m - 1),
        ag_recv=dma(heads, m - 1),
        tap_send=dma(m - 1),
        tap_recv=dma(m - 1),
    )
    anywhere = pl.BlockSpec(memory_space=pl.ANY)
    shape = jax.ShapeDtypeStruct
    whole, maps, sums = pl.pallas_call(
        functools.partial(whole_kernel, (n, m, heads, tok, rows, q), norm),
        in_specs=[anywhere] * 7,
        out_specs=[anywhere] * 3,
        out_shape=[
            shape(mixing_input.shape, bf16),
            shape((heads, 4 * LANES, LANES), wire),
            shape((heads, SEG, LANES), f32),
        ],
        scratch_shapes=[scratch],
        compiler_params=pltpu.CompilerParams(
            collective_id=0, has_side_effects=True, vmem_limit_bytes=56 * 1024 * 1024
        ),
        name="heads_and_exchange",
    )(mixing_input, cotangent, filter_taps, recurrence_gate_map, input_gate_map,
      decay_logit_param, spike_decay)
    outs = [
        shape(mixing_input.shape, bf16),
        shape(recurrence_gate_map.shape, f32),
        shape(recurrence_gate_map.shape, f32),
        shape((4, heads * LANES), f32),
    ]
    room = lambda a: pltpu.VMEM(a.shape, a.dtype)
    return pl.pallas_call(
        functools.partial(finish_kernel, heads),
        in_specs=[anywhere] * 3,
        out_specs=[anywhere] * 4,
        out_shape=outs,
        scratch_shapes=[room(whole), room(maps), room(sums), room(outs[1]), room(outs[2]), room(outs[3]), dma(7)],
        compiler_params=pltpu.CompilerParams(vmem_limit_bytes=56 * 1024 * 1024),
        name="finish",
    )(whole, maps, sums)


def solution(mesh):
    return jax.shard_map(
        body,
        mesh=mesh,
        in_specs=(
            P("dp", "sp", None),
            P("dp", "sp", None),
            P(None, "sp"),
            P(None, "sp", None, None),
            P(None, "sp", None, None),
            P(None, "sp"),
            P("dp", "sp", None),
        ),
        out_specs=(
            P("dp", "sp", None),
            P(None, "sp", None, None),
            P(None, "sp", None, None),
            P(None, "sp"),
        ),
        check_vma=False,
    )
```
